32 devices in a mesh: sp: 16 (over z, y, x), tp: 2 (over core).
Axes of the slice: x: 2, y: 2, z: 4, core: 2. Of those that a mesh axis runs over, the one named last changes fastest.
Arguments:
- queries: bfloat16 [4096, 2048], P('sp', 'tp'), may hold values from -6 to 6
- keys: bfloat16 [4096, 2048], P('sp', 'tp'), may hold values from -6 to 6
- hidden: bfloat16 [4096, 2048], P('sp'), may hold values from -6 to 6
- value_weight: bfloat16 [2048, 2048], P(None, 'tp'), may hold values from -0.125 to 0.125
- beta_pre: float32 [4096, 16], P('sp', 'tp'), may hold values from -9 to 3
- decay_pre: float32 [4096, 16], P('sp', 'tp'), may hold values from -5 to 4
- decay_rate: float32 [16], P('tp'), may hold values from 0 to 0.06
- out_grad: bfloat16 [4096, 2048], P('sp', 'tp'), may hold values from -6 to 6
Outputs:
- d_queries: bfloat16 [4096, 2048], P('sp', 'tp')
- d_keys: bfloat16 [4096, 2048], P('sp', 'tp')
- d_beta: float32 [4096, 16], P('sp', 'tp')
- d_decay: float32 [4096, 16], P('sp', 'tp')
- d_hidden: bfloat16 [4096, 2048], P(('sp', 'tp'))
- d_weight: float32 [2048, 2048], P('sp', 'tp')
The draws below stay inside these ranges and needn't reach their ends.
All inputs are finite; a program needn't handle non-finite values.
Results may differ from the reference program's by a relative error of at most 0.022.
Values may be sent and summed in bfloat16 or wider, within the bound.
A program may use at most 256 MiB of HBM per device.

```python
import jax
import jax.numpy as jnp
from jax import lax

D = 2048
HEADS = 16
DK = 128
DV = 128
BLOCK = 64
TOK_DEV = 256
TOKENS = 4096
HEADS_DEV = 8


def slow_heads(key):
    order = jax.random.permutation(jax.random.fold_in(key, 11), HEADS)
    return order < HEADS // 2


def noise_field(key, shape):
    return jnp.clip(jax.random.normal(key, shape, jnp.float32), -3.0, 3.0)


def draw_decay_rate(key, part):
    slow = slow_heads(key)
    pick = jax.random.uniform(jax.random.fold_in(key, 12), (HEADS,), jnp.float32)
    return jnp.where(slow, (0.3 + 1.2 * pick) / TOKENS, 0.02 + 0.04 * pick)


def draw_beta_pre(key, part):
    slow = slow_heads(key)
    noise = noise_field(jax.random.fold_in(key, 13), (TOKENS, HEADS))
    return noise + jnp.where(slow, -5.5, 0.0)[None, :]


def draw_decay_pre(key, part):
    offset = jax.random.uniform(jax.random.fold_in(key, 21), (TOKENS // TOK_DEV, HEADS), jnp.float32, -2.0, 1.0)
    noise = noise_field(jax.random.fold_in(key, 22), (TOKENS, HEADS))
    return noise + jnp.repeat(offset, TOK_DEV, axis=0)


def shard_levels(key, dims, cuts, least, high):
    loudness = 1.0
    for dim, blocks in cuts:
        steps = jax.random.uniform(jax.random.fold_in(jax.random.fold_in(key, 6), dim), (blocks,), jnp.float32, least / len(cuts), high / len(cuts))
        loudness = loudness * jnp.repeat(jnp.exp(steps), dims[dim] // blocks).reshape((-1,) + (1,) * (len(dims) - 1 - dim))
    return loudness


def normal_values(stream_key, extent, scale, reach, cuts=(), kind=jnp.bfloat16):
    factor_of = shard_levels(stream_key, extent, cuts, -0.22, 0.18) if cuts else 1.0
    array = jax.random.normal(stream_key, extent, jnp.float32) * scale * factor_of
    return jnp.minimum(jnp.maximum(array, -reach), reach).astype(kind)


def setup_inputs(seed: int = 0) -> dict:
    arg_keys = jax.random.split(jax.random.key(seed), 9)
    return {
        "queries": normal_values(arg_keys[0], (TOKENS, HEADS * DK), 1.0, 6.0, ((0, 16), (1, 2))),
        "keys": normal_values(arg_keys[1], (TOKENS, HEADS * DK), 1.0, 6.0, ((0, 16), (1, 2))),
        "hidden": normal_values(arg_keys[2], (TOKENS, D), 1.0, 6.0, ((0, 16),)),
        "value_weight": normal_values(arg_keys[3], (D, HEADS * DV), D ** -0.5, 0.125, ((1, 2),)),
        "beta_pre": draw_beta_pre(jax.random.fold_in(arg_keys[8], 71), 0),
        "decay_pre": draw_decay_pre(jax.random.fold_in(arg_keys[8], 71), 0),
        "decay_rate": draw_decay_rate(jax.random.fold_in(arg_keys[8], 71), 0),
        "out_grad": normal_values(arg_keys[7], (TOKENS, HEADS * DV), 1.0, 6.0, ((0, 16), (1, 2))),
    }


highest = lax.Precision.HIGHEST
norm_floor = 16.0

def to_blocks(tensor, blocks):
    shaped = tensor.reshape((blocks, BLOCK) + tensor.shape[1:])
    return jnp.moveaxis(shaped, 1, 2)

def block_setup(key_raw, beta_pre, decay_pre, rate):
    blocks = key_raw.shape[0] // BLOCK
    key_unit = key_raw * lax.rsqrt(lax.optimization_barrier(jnp.sum(key_raw * key_raw, axis=-1, keepdims=True)) + norm_floor)
    write_rate = jax.nn.sigmoid(beta_pre)
    log_decay = -rate[None, :] * jax.nn.softplus(decay_pre)
    key_blocks = to_blocks(key_unit, blocks)
    rate_blocks = to_blocks(write_rate, blocks)
    log_sums = jnp.cumsum(to_blocks(log_decay, blocks), axis=-1)
    position = jnp.arange(BLOCK)
    inclusive = position[:, None] >= position[None, :]
    strict = position[:, None] > position[None, :]
    spread = log_sums[..., :, None] - log_sums[..., None, :]
    decay_mask = jnp.where(inclusive, jnp.exp(jnp.where(inclusive, spread, 0.0)), 0.0)
    key_gram = jnp.einsum('nhid,nhjd->nhij', key_blocks, key_blocks, precision=highest)
    lower_part = jnp.where(strict, rate_blocks[..., :, None] * key_gram * decay_mask, 0.0)
    system = jnp.eye(BLOCK, dtype=jnp.float32) + lower_part
    return (key_blocks, rate_blocks, log_sums, decay_mask, system)

def span_pieces(query_raw, key_raw, values, beta_pre, decay_pre, rate):
    key_blocks, rate_blocks, log_sums, decay_mask, system = block_setup(key_raw, beta_pre, decay_pre, rate)
    blocks = key_blocks.shape[0]
    query_unit = query_raw * lax.rsqrt(lax.optimization_barrier(jnp.sum(query_raw * query_raw, axis=-1, keepdims=True)) + norm_floor)
    query_unit = query_unit * query_raw.shape[-1] ** (-0.5)
    query_blocks = to_blocks(query_unit, blocks)
    value_blocks = to_blocks(values, blocks)
    block_gain = jnp.exp(log_sums)
    right_side = jnp.concatenate([rate_blocks[..., None] * value_blocks, (rate_blocks * block_gain)[..., None] * key_blocks], axis=-1)
    solved = jax.scipy.linalg.solve_triangular(system, right_side, lower=True, unit_diagonal=True)
    value_size = values.shape[-1]
    query_key = jnp.einsum('nhid,nhjd->nhij', query_blocks, key_blocks, precision=highest) * decay_mask
    query_decayed = query_blocks * block_gain[..., None]
    key_decayed = key_blocks * jnp.exp(log_sums[..., -1:] - log_sums)[..., None]
    return (solved[..., :value_size], solved[..., value_size:], query_key, query_decayed, key_decayed, block_gain[..., -1])

def span_run(query_raw, key_raw, values, beta_pre, decay_pre, rate, carry_state):
    pieces = span_pieces(query_raw, key_raw, values, beta_pre, decay_pre, rate)

    def advance(current, inputs):
        new_values, key_sweep, query_key, query_decayed, key_decayed, end_gain = inputs
        written = new_values - jnp.einsum('hcd,hde->hce', key_sweep, current, precision=highest)
        output = jnp.einsum('hcd,hde->hce', query_decayed, current, precision=highest)
        output = output + jnp.einsum('hij,hje->hie', query_key, written, precision=highest)
        current = end_gain[:, None, None] * current + jnp.einsum('hcd,hce->hde', key_decayed, written, precision=highest)
        return (current, output)
    final, outputs = lax.scan(advance, carry_state, pieces)
    outputs = jnp.moveaxis(outputs, 2, 1)
    return (outputs.reshape(query_raw.shape[0], outputs.shape[2], outputs.shape[3]), final)

def reference(queries, keys, hidden, value_weight, beta_pre, decay_pre, decay_rate, out_grad):
    values = jnp.dot(hidden.astype(jnp.float32), value_weight.astype(jnp.float32), preferred_element_type=jnp.float32).astype(jnp.bfloat16)
    spans = TOKENS // TOK_DEV

    def by_span(tensor, width):
        return tensor.astype(jnp.float32).reshape(spans, TOK_DEV, HEADS, width)
    query_spans = by_span(queries, DK)
    key_spans = by_span(keys, DK)
    value_spans = by_span(values, DV)
    grad_spans = by_span(out_grad, DV)
    beta_spans = beta_pre.reshape(spans, TOK_DEV, HEADS)
    decay_spans = decay_pre.reshape(spans, TOK_DEV, HEADS)
    zero_state = jnp.zeros((HEADS, DK, DV), jnp.float32)

    def local_run(query_raw, key_raw, span_values, span_beta, span_decay, start_state):
        return span_run(query_raw, key_raw, span_values, span_beta, span_decay, decay_rate, start_state)

    def forward(current, inputs):
        outputs, final = local_run(*inputs, current)
        return (final, current)
    _, starts = lax.scan(forward, zero_state, (query_spans, key_spans, value_spans, beta_spans, decay_spans))

    def backward(state_grad, inputs):
        query_raw, key_raw, span_values, span_beta, span_decay, span_grad, start_state = inputs
        primal = (query_raw, key_raw, span_values, span_beta, span_decay)
        _, pullback = jax.vjp(local_run, *primal, start_state)
        grad_query, grad_key, grad_value, grad_beta, grad_decay, grad_state = pullback((span_grad, state_grad))
        _, pull_zero = jax.vjp(local_run, *primal, zero_state)
        own_value = pull_zero((span_grad, jnp.zeros_like(zero_state)))[2]
        return (grad_state, (grad_query, grad_key, grad_value, grad_beta, grad_decay, own_value))
    _, grads = lax.scan(backward, zero_state, (query_spans, key_spans, value_spans, beta_spans, decay_spans, grad_spans, starts), reverse=True)
    grad_query, grad_key, value_total, grad_beta, grad_decay, value_local = grads
    d_queries = grad_query.reshape(TOKENS, HEADS * DK).astype(jnp.bfloat16)
    d_keys = grad_key.reshape(TOKENS, HEADS * DK).astype(jnp.bfloat16)
    d_beta = grad_beta.reshape(TOKENS, HEADS)
    d_decay = grad_decay.reshape(TOKENS, HEADS)
    value_carried = value_total - value_local
    local_grad = value_local.reshape(TOKENS, HEADS * DV).astype(jnp.bfloat16)
    carried_grad = value_carried.reshape(TOKENS, HEADS * DV).astype(jnp.bfloat16)
    d_weight = jnp.dot(hidden.T.astype(jnp.float32), local_grad.astype(jnp.float32), preferred_element_type=jnp.float32)
    d_weight = d_weight + jnp.dot(hidden.T.astype(jnp.float32), carried_grad.astype(jnp.float32), preferred_element_type=jnp.float32)
    group_width = HEADS_DEV * DV
    total = jnp.zeros((TOKENS, D), jnp.float32)
    for group in range(HEADS // HEADS_DEV):
        columns = slice(group * group_width, (group + 1) * group_width)
        weight_part = value_weight[:, columns].T
        partial_sum = jnp.dot(local_grad[:, columns].astype(jnp.float32), weight_part.astype(jnp.float32), preferred_element_type=jnp.float32)
        partial_sum = partial_sum + jnp.dot(carried_grad[:, columns].astype(jnp.float32), weight_part.astype(jnp.float32), preferred_element_type=jnp.float32)
        rounded = lax.optimization_barrier(partial_sum.astype(jnp.bfloat16))
        total = total + rounded.astype(jnp.float32)
    d_hidden = total.astype(jnp.bfloat16)
    return (d_queries, d_keys, d_beta, d_decay, d_hidden, d_weight)
```

```python
import functools

import jax
import jax.numpy as jnp
from jax import lax
from jax.experimental import pallas as pl
from jax.experimental.pallas import tpu as pltpu
from jax.sharding import PartitionSpec as P

f32 = jnp.float32
bf16 = jnp.bfloat16
norm_floor = 16.0


def mm(a, b, ca, cb):
    return lax.dot_general(
        a.astype(bf16), b.astype(bf16), (((ca,), (cb,)), ((), ())), preferred_element_type=f32
    )


def nn(a, b):
    return mm(a, b, 1, 0)


def nt(a, b):
    return mm(a, b, 1, 1)


def tn(a, b):
    return mm(a, b, 0, 0)


def nn3(a, b):
    a_hi, b_hi = a.astype(bf16), b.astype(bf16)
    a_lo, b_lo = a - a_hi.astype(f32), b - b_hi.astype(f32)
    return nn(a_hi, b_hi) + (nn(a_hi, b_lo) + nn(a_lo, b_hi))


def invert_unit_lower(low):
    size = low.shape[0]
    base = min(size, 128)
    ii = lax.broadcasted_iota(jnp.int32, (base, base), 0)
    jj = lax.broadcasted_iota(jnp.int32, (base, base), 1)
    masks = []
    width = 1
    while width < base:
        masks.append((ii // (2 * width) == jj // (2 * width)) & (ii // width != jj // width))
        width *= 2
    parts = []
    for start in range(0, size, base):
        block = low[start : start + base, start : start + base]
        inverse = jnp.where(ii == jj, 1.0, 0.0) - jnp.where(masks[0], block, 0.0)
        parts.append([block, inverse])
    for mask in masks[1:]:
        for part in parts:
            off = jnp.where(mask, part[0], 0.0)
            part[1] = part[1] - nn3(part[1], nn3(off, part[1]))
    inverses = [part[1] for part in parts]
    while len(inverses) > 1:
        joined = []
        width = inverses[0].shape[0]
        for pair in range(0, len(inverses), 2):
            first, second = inverses[pair], inverses[pair + 1]
            row = (pair + 1) * width
            cross = low[row : row + width, row - width : row]
            corner = -nn3(second, nn3(cross, first))
            top = jnp.concatenate([first, jnp.zeros_like(first)], axis=1)
            joined.append(
                jnp.concatenate([top, jnp.concatenate([corner, second], axis=1)], axis=0)
            )
        inverses = joined
    return inverses[0]


def unit(raw):
    return lax.rsqrt(jnp.sum(raw * raw, axis=-1, keepdims=True) + norm_floor)


def order(size):
    ii = lax.broadcasted_iota(jnp.int32, (size, size), 0)
    jj = lax.broadcasted_iota(jnp.int32, (size, size), 1)
    return ii >= jj, ii > jj


def first_phase(qr, kr, v, do, b, gc, gr, ge):
    width = qr.shape[1]
    q = qr * (unit(qr) * width ** (-0.5))
    k = kr * unit(kr)
    inclusive, strict = order(qr.shape[0])
    mask = jnp.where(inclusive, jnp.exp(jnp.minimum(gc - gr, 0.0)), 0.0)
    low = jnp.where(strict, b * nt(k, k) * mask, 0.0)
    inverse = invert_unit_lower(low)
    eg = jnp.exp(gc)
    kd = k * jnp.exp(ge - gc)
    uw = nn(inverse, jnp.concatenate([b * v, (b * eg) * k], axis=1))
    qk = nt(q, k) * mask
    moved = tn(kd, uw)
    ii = lax.broadcasted_iota(jnp.int32, (width, width), 0)
    jj = lax.broadcasted_iota(jnp.int32, (width, width), 1)
    dv = v.shape[1]
    offset = moved[:, :dv]
    transition = jnp.where(ii == jj, jnp.exp(ge), 0.0) - moved[:, dv:]
    dw0 = tn(qk, do)
    own = tn(q * eg, do) - tn(uw[:, dv:], dw0)
    return inverse, uw, dw0, transition, offset, own


def value_phase(kr, inverse, dw0, end, b, gc, ge):
    kd = kr * (unit(kr) * jnp.exp(ge - gc))
    return tn(inverse, dw0 + nn(kd, end))


def last_phase(qr, kr, v, do, uw, dr, start, end, b, gc, gr, ge):
    width = qr.shape[1]
    dv = v.shape[1]
    rq, rk = unit(qr), unit(kr)
    scale = width ** (-0.5)
    q = qr * (rq * scale)
    k = kr * rk
    inclusive, strict = order(qr.shape[0])
    mask = jnp.where(inclusive, jnp.exp(jnp.minimum(gc - gr, 0.0)), 0.0)
    gram = jnp.where(strict, nt(k, k) * mask, 0.0)
    qk = nt(q, k) * mask
    eg = jnp.exp(gc)
    ekd = jnp.exp(ge - gc)
    rest = v - eg * nn(k, start)
    written = uw[:, :dv] - nn(uw[:, dv:], start)
    dp = nt(do, written)
    dqd = nt(do, start) * eg
    dkd = nt(written, end) * ekd
    dl = -nt(dr, written)
    dkg = nt(dr, start) * (-b * eg)
    dlg = dl * gram
    db = jnp.sum(dr * rest, axis=1, keepdims=True) + jnp.sum(dlg, axis=1, keepdims=True)
    dg = jnp.where(strict, dl * b * mask, 0.0)
    dqk = dp * mask
    logs = dlg * b + dp * qk
    dq = nn(dqk, k) + dqd
    dk = tn(dqk, q) + nn(dg, k) + tn(dg, k) + dkg + dkd
    kept = jnp.sum(dkd * k, axis=1, keepdims=True)
    gcol = jnp.sum(logs, axis=1, keepdims=True) + jnp.sum(dqd * q + dkg * k, axis=1, keepdims=True) - kept
    last = jnp.sum(kept, axis=0, keepdims=True) + jnp.exp(ge) * jnp.sum(
        jnp.sum(start * end, axis=1, keepdims=True), axis=0, keepdims=True
    )
    rows = lax.broadcasted_iota(jnp.int32, gcol.shape, 0)
    gcol = gcol + jnp.where(rows == gcol.shape[0] - 1, last, 0.0)
    grow = jnp.sum(logs, axis=0, keepdims=True)
    dqr = (rq * scale) * (dq - qr * (rq * rq * jnp.sum(qr * dq, axis=1, keepdims=True)))
    dkr = rk * (dk - kr * (rk * rk * jnp.sum(kr * dk, axis=1, keepdims=True)))
    return dqr, dkr, db, gcol, grow


def pick(ref, head):
    table = ref[...]
    lane = lax.broadcasted_iota(jnp.int32, table.shape, 1)
    return jnp.sum(jnp.where(lane == head, table, 0.0), axis=1, keepdims=True)


def put(ref, head, column):
    lane = lax.broadcasted_iota(jnp.int32, ref.shape, 1)
    ref[...] = jnp.where(lane == head, column, ref[...])


def gains(g_ref, row_ref, head):
    gr = row_ref[0]
    return pick(g_ref, head), gr, gr[:, gr.shape[1] - 1 :]


def first_kernel(q, k, v, do, b, g, row, inv_o, uw_o, dw_o, t_o, off_o, own_o):
    head = pl.program_id(0)
    gc, gr, ge = gains(g, row, head)
    inverse, uw, dw0, transition, offset, own = first_phase(
        q[...].astype(f32), k[...].astype(f32), v[...].astype(f32), do[...].astype(f32),
        pick(b, head), gc, gr, ge,
    )
    inv_o[0] = inverse.astype(inv_o.dtype)
    uw_o[0] = uw
    dw_o[0] = dw0
    t_o[0] = transition.astype(bf16)
    off_o[0] = offset.astype(bf16)
    own_o[0] = own.astype(bf16)


def value_kernel(k, inv, dw, end, b, g, row, dr_o, dv_o):
    head = pl.program_id(0)
    gc, gr, ge = gains(g, row, head)
    bc = pick(b, head)
    dr = value_phase(k[...].astype(f32), inv[0], dw[0], end[0], bc, gc, ge)
    dr_o[0] = dr
    dv_o[...] = (bc * dr).astype(bf16)


def last_kernel(q, k, v, do, uw, dr, start, end, b, g, row, dq_o, dk_o, db_o, gc_o, gr_o):
    head = pl.program_id(0)
    gc, gr, ge = gains(g, row, head)
    dqr, dkr, db, gcol, grow = last_phase(
        q[...].astype(f32), k[...].astype(f32), v[...].astype(f32), do[...].astype(f32),
        uw[0], dr[0], start[0].astype(f32), end[0].astype(f32), pick(b, head), gc, gr, ge,
    )
    dq_o[...] = dqr.astype(bf16)
    dk_o[...] = dkr.astype(bf16)

    @pl.when(head == 0)
    def _():
        db_o[...] = jnp.zeros_like(db_o)
        gc_o[...] = jnp.zeros_like(gc_o)

    put(db_o, head, db)
    put(gc_o, head, gcol)
    gr_o[0] = grow


def scan_kernel(count, t, off, own, start_o, end_o):
    shape = off.shape[1:]

    def split(a, b, ca):
        hi = b.astype(bf16)
        return mm(a, hi, ca, 0) + mm(a, b - hi.astype(f32), ca, 0)

    def step(i, carry):
        state, grad = carry
        j = count - 1 - i
        start_o[i] = state.astype(bf16)
        end_o[j] = grad.astype(bf16)
        state = split(t[i], state, 1) + off[i].astype(f32)
        grad = split(t[j], grad, 0) + own[j].astype(f32)
        return state, grad

    zero = jnp.zeros(shape, f32)
    lax.fori_loop(0, count, step, (zero, zero))


def per_device(queries, keys, hidden, value_weight, beta_pre, decay_pre, decay_rate, out_grad):
    heads = decay_rate.shape[0]
    length, dk = queries.shape[0], queries.shape[1] // heads
    dv = value_weight.shape[1] // heads
    count = lax.axis_size("sp")
    parts = count // heads
    cols = dv // parts

    values = jnp.dot(hidden, value_weight, preferred_element_type=f32).astype(bf16)
    beta = jax.nn.sigmoid(beta_pre)
    log_decay = -decay_rate[None, :] * jax.nn.softplus(decay_pre)
    inclusive = jnp.tril(jnp.ones((length, length), f32))
    sums = jnp.dot(inclusive, log_decay, precision=lax.Precision.HIGHEST)
    sums_row = sums.T.reshape(heads, 1, length)

    wide = lambda n: pl.BlockSpec((length, n), lambda h: (0, h))
    per_head = lambda r, c: pl.BlockSpec((1, r, c), lambda h: (h, 0, 0))
    table = pl.BlockSpec((length, heads), lambda h: (0, 0))
    shape = jax.ShapeDtypeStruct
    params = pltpu.CompilerParams(dimension_semantics=("arbitrary",))

    inverse, uw, dw0, transition, offset, own = pl.pallas_call(
        first_kernel,
        grid=(heads,),
        in_specs=[wide(dk), wide(dk), wide(dv), wide(dv), table, table, per_head(1, length)],
        out_specs=[
            per_head(length, length), per_head(length, dv + dk), per_head(length, dv),
            per_head(dk, dk), per_head(dk, dv), per_head(dk, dv),
        ],
        out_shape=[
            shape((heads, length, length), bf16), shape((heads, length, dv + dk), f32),
            shape((heads, length, dv), f32), shape((heads, dk, dk), bf16),
            shape((heads, dk, dv), bf16), shape((heads, dk, dv), bf16),
        ],
        compiler_params=params,
        name="first",
    )(queries, keys, values, out_grad, beta, sums, sums_row)

    def by_owner(a):
        a = a.reshape(heads, dk, parts, cols)
        return jnp.moveaxis(a, 2, 1).reshape(count, dk, cols)

    packed = jnp.concatenate(
        [jnp.repeat(transition, parts, axis=0), by_owner(offset), by_owner(own)], axis=2
    )
    got = lax.all_to_all(packed, "sp", 0, 0, tiled=True)
    starts, ends = pl.pallas_call(
        functools.partial(scan_kernel, count),
        out_shape=[shape((count, dk, cols), bf16), shape((count, dk, cols), bf16)],
        name="scan",
    )(got[:, :, :dk], got[:, :, dk : dk + cols], got[:, :, dk + cols :])
    back = lax.all_to_all(jnp.concatenate([starts, ends], axis=2), "sp", 0, 0, tiled=True)
    back = jnp.moveaxis(back.reshape(heads, parts, dk, 2, cols), 1, 3).reshape(heads, dk, 2, dv)
    start, end = back[:, :, 0], back[:, :, 1]

    dr, grad_values = pl.pallas_call(
        value_kernel,
        grid=(heads,),
        in_specs=[
            wide(dk), per_head(length, length), per_head(length, dv), per_head(dk, dv),
            table, table, per_head(1, length),
        ],
        out_specs=[per_head(length, dv), wide(dv)],
        out_shape=[shape((heads, length, dv), f32), shape((length, heads * dv), bf16)],
        compiler_params=params,
        name="value",
    )(keys, inverse, dw0, end, beta, sums, sums_row)

    partial_weight = lax.dot_general(
        hidden, grad_values, (((0,), (0,)), ((), ())), preferred_element_type=f32
    )
    d_weight = lax.psum_scatter(
        partial_weight.astype(bf16), "sp", scatter_dimension=0, tiled=True
    ).astype(f32)
    partial_hidden = lax.dot_general(
        grad_values, value_weight, (((1,), (1,)), ((), ())), preferred_element_type=f32
    )
    d_hidden = lax.psum_scatter(
        partial_hidden.astype(bf16), "tp", scatter_dimension=0, tiled=True
    )

    d_queries, d_keys, db, gcol, grow = pl.pallas_call(
        last_kernel,
        grid=(heads,),
        in_specs=[
            wide(dk), wide(dk), wide(dv), wide(dv), per_head(length, dv + dk),
            per_head(length, dv), per_head(dk, dv), per_head(dk, dv),
            table, table, per_head(1, length),
        ],
        out_specs=[wide(dk), wide(dk), table, table, per_head(1, length)],
        out_shape=[
            shape(queries.shape, bf16), shape(keys.shape, bf16), shape((length, heads), f32),
            shape((length, heads), f32), shape((heads, 1, length), f32),
        ],
        compiler_params=params,
        cost_estimate=pl.CostEstimate(
            flops=heads * 13 * 2 * length * length * dk, bytes_accessed=12 << 20, transcendentals=0
        ),
        name="last",
    )(queries, keys, values, out_grad, uw, dr, start, end, beta, sums, sums_row)
    grad_sums = gcol - grow.reshape(heads, length).T
    grad_log = jnp.dot(inclusive.T, grad_sums, precision=lax.Precision.HIGHEST)
    d_decay = grad_log * (-decay_rate[None, :] * jax.nn.sigmoid(decay_pre))
    d_beta = db * beta * (1.0 - beta)
    return (d_queries, d_keys, d_beta, d_decay, d_hidden, d_weight)


def solution(mesh):
    return jax.shard_map(
        per_device,
        mesh=mesh,
        in_specs=(
            P("sp", "tp"), P("sp", "tp"), P("sp", None), P(None, "tp"),
            P("sp", "tp"), P("sp", "tp"), P("tp"), P("sp", "tp"),
        ),
        out_specs=(
            P("sp", "tp"), P("sp", "tp"), P("sp", "tp"), P("sp", "tp"),
            P(("sp", "tp"), None), P("sp", "tp"),
        ),
        check_vma=False,
    )
```

```python
import functools

import jax
import jax.numpy as jnp
from jax import lax
from jax.experimental import pallas as pl
from jax.experimental.pallas import tpu as pltpu
from jax.sharding import PartitionSpec as P


f32 = jnp.float32
bf16 = jnp.bfloat16
norm_floor = 16.0


def mm(a, b, ca, cb):
    return lax.dot_general(
        a.astype(bf16), b.astype(bf16), (((ca,), (cb,)), ((), ())), preferred_element_type=f32
    )


def nn(a, b):
    return mm(a, b, 1, 0)


def nt(a, b):
    return mm(a, b, 1, 1)


def tn(a, b):
    return mm(a, b, 0, 0)


def nn3(a, b):
    a_hi, b_hi = a.astype(bf16), b.astype(bf16)
    a_lo, b_lo = a - a_hi.astype(f32), b - b_hi.astype(f32)
    return nn(a_hi, b_hi) + (nn(a_hi, b_lo) + nn(a_lo, b_hi))


def invert_unit_lower(lows):
    size = lows[0].shape[0]
    base = min(size, 128)
    ii = lax.broadcasted_iota(jnp.int32, (base, base), 0)
    jj = lax.broadcasted_iota(jnp.int32, (base, base), 1)
    masks = []
    width = 1
    while width < base:
        masks.append((ii // (2 * width) == jj // (2 * width)) & (ii // width != jj // width))
        width *= 2
    blocks = [
        low[start : start + base, start : start + base]
        for low in lows
        for start in range(0, size, base)
    ]
    inverses = [jnp.where(ii == jj, 1.0, 0.0) - jnp.where(masks[0], a, 0.0) for a in blocks]
    for mask in masks[1:]:
        inner = [nn3(jnp.where(mask, a, 0.0), inv) for a, inv in zip(blocks, inverses)]
        outer = [nn3(inv, mid) for inv, mid in zip(inverses, inner)]
        inverses = [inv - out for inv, out in zip(inverses, outer)]
    per = size // base
    while per > 1:
        width = size // per
        joined, inner = [], []
        for pair in range(0, len(inverses), 2):
            low = lows[pair // per]
            row = (pair % per + 1) * width
            inner.append(nn3(low[row : row + width, row - width : row], inverses[pair]))
        for pair in range(0, len(inverses), 2):
            first, second = inverses[pair], inverses[pair + 1]
            corner = -nn3(second, inner[pair // 2])
            top = jnp.concatenate([first, jnp.zeros_like(first)], axis=1)
            joined.append(
                jnp.concatenate([top, jnp.concatenate([corner, second], axis=1)], axis=0)
            )
        inverses = joined
        per //= 2
    return inverses


def unit(raw):
    return lax.rsqrt(jnp.sum(raw * raw, axis=-1, keepdims=True) + norm_floor)


def order(size):
    ii = lax.broadcasted_iota(jnp.int32, (size, size), 0)
    jj = lax.broadcasted_iota(jnp.int32, (size, size), 1)
    return ii >= jj, ii > jj


def first_phase_group(inputs):
    prepared = [first_before(*one) for one in inputs]
    inverses = invert_unit_lower([one[0] for one in prepared])
    return [
        first_after(inverse, one[1], *given)
        for inverse, one, given in zip(inverses, prepared, inputs)
    ]


def first_before(qr, kr, v, do, b, gc, gr, ge):
    k = kr * unit(kr)
    inclusive, strict = order(qr.shape[0])
    mask = jnp.where(inclusive, jnp.exp(jnp.minimum(gc - gr, 0.0)), 0.0)
    return jnp.where(strict, b * nt(k, k) * mask, 0.0), mask


def first_after(inverse, mask, qr, kr, v, do, b, gc, gr, ge):
    width = qr.shape[1]
    q = qr * (unit(qr) * width ** (-0.5))
    k = kr * unit(kr)
    eg = jnp.exp(gc)
    kd = k * jnp.exp(ge - gc)
    uw = nn(inverse, jnp.concatenate([b * v, (b * eg) * k], axis=1))
    qk = nt(q, k) * mask
    moved = tn(kd, uw)
    ii = lax.broadcasted_iota(jnp.int32, (width, width), 0)
    jj = lax.broadcasted_iota(jnp.int32, (width, width), 1)
    dv = v.shape[1]
    offset = moved[:, :dv]
    transition = jnp.where(ii == jj, jnp.exp(ge), 0.0) - moved[:, dv:]
    dw0 = tn(qk, do)
    own = tn(q * eg, do) - tn(uw[:, dv:], dw0)
    return inverse, uw, dw0, transition, offset, own


def value_phase(kr, inverse, dw0, end, gc, ge):
    kd = kr * (unit(kr) * jnp.exp(ge - gc))
    return tn(inverse, dw0 + nn(kd, end))


def last_phase(qr, kr, v, do, uw, dr, start, end, b, gc, gr, ge):
    width = qr.shape[1]
    dv = v.shape[1]
    rq, rk = unit(qr), unit(kr)
    scale = width ** (-0.5)
    q = qr * (rq * scale)
    k = kr * rk
    inclusive, strict = order(qr.shape[0])
    mask = jnp.where(inclusive, jnp.exp(jnp.minimum(gc - gr, 0.0)), 0.0)
    gram = jnp.where(strict, nt(k, k) * mask, 0.0)
    qk = nt(q, k) * mask
    eg = jnp.exp(gc)
    ekd = jnp.exp(ge - gc)
    rest = v - eg * nn(k, start)
    written = uw[:, :dv] - nn(uw[:, dv:], start)
    dp = nt(do, written)
    dqd = nt(do, start) * eg
    dkd = nt(written, end) * ekd
    dl = -nt(dr, written)
    dkg = nt(dr, start) * (-b * eg)
    dlg = dl * gram
    db = jnp.sum(dr * rest, axis=1, keepdims=True) + jnp.sum(dlg, axis=1, keepdims=True)
    dg = jnp.where(strict, dl * b * mask, 0.0)
    dqk = dp * mask
    logs = dlg * b + dp * qk
    dq = nn(dqk, k) + dqd
    dk = tn(dqk, q) + nn(dg, k) + tn(dg, k) + dkg + dkd
    kept = jnp.sum(dkd * k, axis=1, keepdims=True)
    gcol = jnp.sum(logs, axis=1, keepdims=True) + jnp.sum(dqd * q + dkg * k, axis=1, keepdims=True) - kept
    last = jnp.sum(kept, axis=0, keepdims=True) + jnp.exp(ge) * jnp.sum(
        jnp.sum(start * end, axis=1, keepdims=True), axis=0, keepdims=True
    )
    rows = lax.broadcasted_iota(jnp.int32, gcol.shape, 0)
    gcol = gcol + jnp.where(rows == gcol.shape[0] - 1, last, 0.0)
    grow = jnp.sum(logs, axis=0, keepdims=True)
    dqr = (rq * scale) * (dq - qr * (rq * rq * jnp.sum(qr * dq, axis=1, keepdims=True)))
    dkr = rk * (dk - kr * (rk * rk * jnp.sum(kr * dk, axis=1, keepdims=True)))
    return dqr, dkr, db, gcol, grow


def pick(ref, head):
    table = ref[...]
    lane = lax.broadcasted_iota(jnp.int32, table.shape, 1)
    return jnp.sum(jnp.where(lane == head, table, 0.0), axis=1, keepdims=True)


def put(ref, head, column):
    lane = lax.broadcasted_iota(jnp.int32, ref.shape, 1)
    ref[...] = jnp.where(lane == head, column, ref[...])


def gains(g_ref, row_ref, head):
    gr = row_ref[...]
    return pick(g_ref, head), gr, gr[:, gr.shape[1] - 1 :]


def lanes(ref, i, group):
    width = ref.shape[1] // group
    return ref.at[:, i * width : (i + 1) * width]


def first_kernel(group, q, k, v, do, b, g, row, inv_o, uw_o, dw_o, t_o, off_o, own_o):
    results = []
    for i in range(group):
        head = pl.program_id(0) * group + i
        gc, gr, ge = gains(g, row.at[i], head)
        results.append(
            [lanes(a, i, group)[...].astype(f32) for a in (q, k, v, do)]
            + [pick(b, head), gc, gr, ge]
        )
    results = first_phase_group(results)
    for i in range(group):
        inverse, uw, dw0, transition, offset, own = results[i]
        inv_o[i] = inverse.astype(inv_o.dtype)
        uw_o[i] = uw
        dw_o[i] = dw0
        t_o[i] = transition.astype(bf16)
        off_o[i] = offset.astype(bf16)
        own_o[i] = own.astype(bf16)


def value_kernel(group, k, inv, dw, end, b, g, row, dr_o, dv_o):
    for i in range(group):
        head = pl.program_id(0) * group + i
        gc, _, ge = gains(g, row.at[i], head)
        bc = pick(b, head)
        dr = value_phase(lanes(k, i, group)[...].astype(f32), inv[i], dw[i], end[i], gc, ge)
        dr_o[i] = dr
        lanes(dv_o, i, group)[...] = (bc * dr).astype(bf16)


def last_kernel(group, q, k, v, do, uw, dr, start, end, b, g, row, dq_o, dk_o, db_o, gc_o, gr_o):
    @pl.when(pl.program_id(0) == 0)
    def _():
        db_o[...] = jnp.zeros_like(db_o)
        gc_o[...] = jnp.zeros_like(gc_o)

    for i in range(group):
        head = pl.program_id(0) * group + i
        gc, gr, ge = gains(g, row.at[i], head)
        raw = [lanes(a, i, group)[...].astype(f32) for a in (q, k, v, do)]
        dqr, dkr, db, gcol, grow = last_phase(
            *raw, uw[i], dr[i], start[i].astype(f32), end[i].astype(f32), pick(b, head), gc, gr, ge
        )
        lanes(dq_o, i, group)[...] = dqr.astype(bf16)
        lanes(dk_o, i, group)[...] = dkr.astype(bf16)
        put(db_o, head, db)
        put(gc_o, head, gcol)
        gr_o[i] = grow


def scan_kernel(count, t, off, own, start_o, end_o):
    shape = off.shape[1:]

    def split(a, b, ca):
        hi = b.astype(bf16)
        return mm(a, hi, ca, 0) + mm(a, b - hi.astype(f32), ca, 0)

    def step(i, carry):
        state, grad = carry
        j = count - 1 - i
        start_o[i] = state.astype(bf16)
        end_o[j] = grad.astype(bf16)
        state = split(t[i], state, 1) + off[i].astype(f32)
        grad = split(t[j], grad, 0) + own[j].astype(f32)
        return state, grad

    zero = jnp.zeros(shape, f32)
    lax.fori_loop(0, count, step, (zero, zero))


def exchange(value, axis, bit):
    count = lax.axis_size(axis)
    return lax.ppermute(value, axis, [(i, i ^ bit) for i in range(count)])


def bit_of(axis, bit):
    return (lax.axis_index(axis) >> bit) & 1


class Halving:
    def __init__(self, hidden, grads, bits, sequence):
        self.grads, self.sequence = grads, sequence
        self.length, self.rows, self.count = hidden.shape[0], hidden.shape[1], 1 << bits
        self.left = sorted(range(bits), reverse=True)
        self.axis = 1 + self.left.index(sequence[0])
        self.mine = bit_of("sp", sequence[0])
        self.split = hidden.reshape((self.length,) + (2,) * bits + (self.rows // self.count,))
        self.send = self.product(1 - self.mine).astype(bf16)

    def product(self, side):
        piece = lax.dynamic_index_in_dim(self.split, side, self.axis, False)
        piece = piece.reshape(self.length, self.rows // 2)
        return lax.dot_general(
            piece, self.grads, (((0,), (0,)), ((), ())), preferred_element_type=f32
        )

    def finish(self, send):
        left = list(self.left)
        got = exchange(send, "sp", 1 << self.sequence[0])
        total = self.product(self.mine) + got.astype(f32)
        left.remove(self.sequence[0])
        for bit in self.sequence[1:]:
            place = left.index(bit)
            mine = bit_of("sp", bit)
            shaped = total.reshape(1 << place, 2, -1, total.shape[-1])
            send = lax.dynamic_index_in_dim(shaped, 1 - mine, 1, False)
            keep = lax.dynamic_index_in_dim(shaped, mine, 1, False)
            got = exchange(send.astype(bf16), "sp", 1 << bit)
            total = keep + got.astype(f32)
            left.remove(bit)
        return total.reshape(self.rows // self.count, -1)


def plan_weight(hidden, grads, count):
    bits = count.bit_length() - 1
    low = bits // 2
    order_a = list(range(bits))
    order_b = order_a[:low][::-1] + order_a[low:]
    order_c = order_a[low:] + order_a[:low]
    width = grads.shape[1]
    cut = max(width * 3 // 8 // 128 * 128, 1)
    groups = [(0, cut, order_a), (cut, 2 * cut, order_b), (2 * cut, width, order_c)]
    return [Halving(hidden, grads[:, lo:hi], bits, seq) for lo, hi, seq in groups]


def reduce_hidden(grads, weight):
    cores = lax.axis_size("tp")
    assert cores == 2
    half = grads.shape[0] // cores
    me = lax.axis_index("tp")

    def product(side):
        rows = lax.dynamic_slice_in_dim(grads, side * half, half, 0)
        return lax.dot_general(
            rows, weight, (((1,), (1,)), ((), ())), preferred_element_type=f32
        ).astype(bf16)

    got = exchange(product(1 - me), "tp", 1)
    return (product(me).astype(f32) + got.astype(f32)).astype(bf16)


def compute(queries, keys, hidden, value_weight, beta_pre, decay_pre, decay_rate, out_grad):
    heads = decay_rate.shape[0]
    length, dk = queries.shape[0], queries.shape[1] // heads
    dv = value_weight.shape[1] // heads
    count = lax.axis_size("sp")
    parts = count // heads
    group = 2 if heads % 2 == 0 else 1
    cols = dv // parts

    values = jnp.dot(hidden, value_weight, preferred_element_type=f32).astype(bf16)
    beta = jax.nn.sigmoid(beta_pre)
    log_decay = -decay_rate[None, :] * jax.nn.softplus(decay_pre)
    inclusive = jnp.tril(jnp.ones((length, length), f32))
    sums = jnp.dot(inclusive, log_decay, precision=lax.Precision.HIGHEST)
    sums_row = sums.T.reshape(heads, 1, length)

    wide = lambda n: pl.BlockSpec((length, group * n), lambda h: (0, h))
    per_head = lambda r, c: pl.BlockSpec((group, r, c), lambda h: (h, 0, 0))
    table = pl.BlockSpec((length, heads), lambda h: (0, 0))
    shape = jax.ShapeDtypeStruct
    params = pltpu.CompilerParams(dimension_semantics=("arbitrary",))

    inverse, uw, dw0, transition, offset, own = pl.pallas_call(
        functools.partial(first_kernel, group),
        grid=(heads // group,),
        in_specs=[wide(dk), wide(dk), wide(dv), wide(dv), table, table, per_head(1, length)],
        out_specs=[
            per_head(length, length), per_head(length, dv + dk), per_head(length, dv),
            per_head(dk, dk), per_head(dk, dv), per_head(dk, dv),
        ],
        out_shape=[
            shape((heads, length, length), bf16), shape((heads, length, dv + dk), f32),
            shape((heads, length, dv), f32), shape((heads, dk, dk), bf16),
            shape((heads, dk, dv), bf16), shape((heads, dk, dv), bf16),
        ],
        compiler_params=params,
        name="first",
    )(queries, keys, values, out_grad, beta, sums, sums_row)

    def by_owner(a):
        a = a.reshape(heads, dk, parts, cols)
        return jnp.moveaxis(a, 2, 1).reshape(count, dk, cols)

    packed = jnp.concatenate(
        [jnp.repeat(transition, parts, axis=0), by_owner(offset), by_owner(own)], axis=2
    )
    got = lax.all_to_all(packed, "sp", 0, 0, tiled=True)
    starts, ends = pl.pallas_call(
        functools.partial(scan_kernel, count),
        out_shape=[shape((count, dk, cols), bf16), shape((count, dk, cols), bf16)],
        name="scan",
    )(got[:, :, :dk], got[:, :, dk : dk + cols], got[:, :, dk + cols :])
    back = lax.all_to_all(jnp.concatenate([starts, ends], axis=2), "sp", 0, 0, tiled=True)
    back = jnp.moveaxis(back.reshape(heads, parts, dk, 2, cols), 1, 3).reshape(heads, dk, 2, dv)
    start, end = back[:, :, 0], back[:, :, 1]

    dr, grad_values = pl.pallas_call(
        functools.partial(value_kernel, group),
        grid=(heads // group,),
        in_specs=[
            wide(dk), per_head(length, length), per_head(length, dv), per_head(dk, dv),
            table, table, per_head(1, length),
        ],
        out_specs=[per_head(length, dv), wide(dv)],
        out_shape=[shape((heads, length, dv), f32), shape((length, heads * dv), bf16)],
        compiler_params=params,
        name="value",
    )(keys, inverse, dw0, end, beta, sums, sums_row)

    plans = plan_weight(hidden, grad_values, count)
    sends, dr, start = lax.optimization_barrier(([plan.send for plan in plans], dr, start))
    d_weight = jnp.concatenate([plan.finish(x) for plan, x in zip(plans, sends)], axis=1)
    d_hidden = reduce_hidden(grad_values, value_weight)

    d_queries, d_keys, db, gcol, grow = pl.pallas_call(
        functools.partial(last_kernel, group),
        grid=(heads // group,),
        in_specs=[
            wide(dk), wide(dk), wide(dv), wide(dv), per_head(length, dv + dk),
            per_head(length, dv), per_head(dk, dv), per_head(dk, dv),
            table, table, per_head(1, length),
        ],
        out_specs=[wide(dk), wide(dk), table, table, per_head(1, length)],
        out_shape=[
            shape(queries.shape, bf16), shape(keys.shape, bf16), shape((length, heads), f32),
            shape((length, heads), f32), shape((heads, 1, length), f32),
        ],
        compiler_params=params,
        cost_estimate=pl.CostEstimate(
            flops=heads * 13 * 2 * length * length * dk, bytes_accessed=12 << 20, transcendentals=0
        ),
        name="last",
    )(queries, keys, values, out_grad, uw, dr, start, end, beta, sums, sums_row)
    grad_sums = gcol - grow.reshape(heads, length).T
    grad_log = jnp.dot(inclusive.T, grad_sums, precision=lax.Precision.HIGHEST)
    d_decay = grad_log * (-decay_rate[None, :] * jax.nn.sigmoid(decay_pre))
    d_beta = db * beta * (1.0 - beta)
    return (d_queries, d_keys, d_beta, d_decay, d_hidden, d_weight)


def solution(mesh):
    return jax.shard_map(
        compute,
        mesh=mesh,
        in_specs=(
            P("sp", "tp"), P("sp", "tp"), P("sp", None), P(None, "tp"),
            P("sp", "tp"), P("sp", "tp"), P("tp"), P("sp", "tp"),
        ),
        out_specs=(
            P("sp", "tp"), P("sp", "tp"), P("sp", "tp"), P("sp", "tp"),
            P(("sp", "tp"), None), P("sp", "tp"),
        ),
        check_vma=False,
    )
```

```python
import functools

import jax
import jax.numpy as jnp
from jax import lax
from jax.experimental import pallas as pl
from jax.experimental.pallas import tpu as pltpu
from jax.sharding import PartitionSpec as P


f32 = jnp.float32
bf16 = jnp.bfloat16
norm_floor = 16.0


def mm(a, b, ca, cb):
    return lax.dot_general(
        a.astype(bf16), b.astype(bf16), (((ca,), (cb,)), ((), ())), preferred_element_type=f32
    )


def nn(a, b):
    return mm(a, b, 1, 0)


def nt(a, b):
    return mm(a, b, 1, 1)


def tn(a, b):
    return mm(a, b, 0, 0)


def nn3(a, b):
    a_hi, b_hi = a.astype(bf16), b.astype(bf16)
    a_lo, b_lo = a - a_hi.astype(f32), b - b_hi.astype(f32)
    return nn(a_hi, b_hi) + (nn(a_hi, b_lo) + nn(a_lo, b_hi))


def invert_unit_lower(lows):
    size = lows[0].shape[0]
    base = min(size, 128)
    ii = lax.broadcasted_iota(jnp.int32, (base, base), 0)
    jj = lax.broadcasted_iota(jnp.int32, (base, base), 1)
    masks = []
    width = 1
    while width < base:
        masks.append((ii // (2 * width) == jj // (2 * width)) & (ii // width != jj // width))
        width *= 2
    blocks = [
        low[start : start + base, start : start + base]
        for low in lows
        for start in range(0, size, base)
    ]
    inverses = [jnp.where(ii == jj, 1.0, 0.0) - jnp.where(masks[0], a, 0.0) for a in blocks]
    for mask in masks[1:]:
        inner = [nn3(jnp.where(mask, a, 0.0), inv) for a, inv in zip(blocks, inverses)]
        outer = [nn3(inv, mid) for inv, mid in zip(inverses, inner)]
        inverses = [inv - out for inv, out in zip(inverses, outer)]
    per = size // base
    while per > 1:
        width = size // per
        joined, inner = [], []
        for pair in range(0, len(inverses), 2):
            low = lows[pair // per]
            row = (pair % per + 1) * width
            inner.append(nn3(low[row : row + width, row - width : row], inverses[pair]))
        for pair in range(0, len(inverses), 2):
            first, second = inverses[pair], inverses[pair + 1]
            corner = -nn3(second, inner[pair // 2])
            top = jnp.concatenate([first, jnp.zeros_like(first)], axis=1)
            joined.append(
                jnp.concatenate([top, jnp.concatenate([corner, second], axis=1)], axis=0)
            )
        inverses = joined
        per //= 2
    return inverses


def unit(raw):
    return lax.rsqrt(jnp.sum(raw * raw, axis=-1, keepdims=True) + norm_floor)


def order(size):
    ii = lax.broadcasted_iota(jnp.int32, (size, size), 0)
    jj = lax.broadcasted_iota(jnp.int32, (size, size), 1)
    return ii >= jj, ii > jj


def first_phase_group(inputs):
    prepared = [first_before(*one) for one in inputs]
    inverses = invert_unit_lower([one[0] for one in prepared])
    return [
        first_after(inverse, one[1], *given)
        for inverse, one, given in zip(inverses, prepared, inputs)
    ]


def first_before(qr, kr, v, do, b, gc, gr, ge):
    k = kr * unit(kr)
    inclusive, strict = order(qr.shape[0])
    mask = jnp.where(inclusive, jnp.exp(jnp.minimum(gc - gr, 0.0)), 0.0)
    return jnp.where(strict, b * nt(k, k) * mask, 0.0), mask


def first_after(inverse, mask, qr, kr, v, do, b, gc, gr, ge):
    width = qr.shape[1]
    q = qr * (unit(qr) * width ** (-0.5))
    k = kr * unit(kr)
    eg = jnp.exp(gc)
    kd = k * jnp.exp(ge - gc)
    uw = nn(inverse, jnp.concatenate([b * v, (b * eg) * k], axis=1))
    qk = nt(q, k) * mask
    moved = tn(kd, uw)
    ii = lax.broadcasted_iota(jnp.int32, (width, width), 0)
    jj = lax.broadcasted_iota(jnp.int32, (width, width), 1)
    dv = v.shape[1]
    offset = moved[:, :dv]
    transition = jnp.where(ii == jj, jnp.exp(ge), 0.0) - moved[:, dv:]
    dw0 = tn(qk, do)
    own = tn(q * eg, do) - tn(uw[:, dv:], dw0)
    return inverse, uw, dw0, transition, offset, own


def value_phase(kr, inverse, dw0, end, gc, ge):
    kd = kr * (unit(kr) * jnp.exp(ge - gc))
    return tn(inverse, dw0 + nn(kd, end))


def last_phase(qr, kr, v, do, uw, dr, start, end, b, gc, gr, ge):
    width = qr.shape[1]
    dv = v.shape[1]
    rq, rk = unit(qr), unit(kr)
    scale = width ** (-0.5)
    q = qr * (rq * scale)
    k = kr * rk
    inclusive, strict = order(qr.shape[0])
    mask = jnp.where(inclusive, jnp.exp(jnp.minimum(gc - gr, 0.0)), 0.0)
    gram = jnp.where(strict, nt(k, k) * mask, 0.0)
    qk = nt(q, k) * mask
    eg = jnp.exp(gc)
    ekd = jnp.exp(ge - gc)
    rest = v - eg * nn(k, start)
    written = uw[:, :dv] - nn(uw[:, dv:], start)
    dp = nt(do, written)
    dqd = nt(do, start) * eg
    dkd = nt(written, end) * ekd
    dl = -nt(dr, written)
    dkg = nt(dr, start) * (-b * eg)
    dlg = dl * gram
    db = jnp.sum(dr * rest, axis=1, keepdims=True) + jnp.sum(dlg, axis=1, keepdims=True)
    dg = jnp.where(strict, dl * b * mask, 0.0)
    dqk = dp * mask
    logs = dlg * b + dp * qk
    dq = nn(dqk, k) + dqd
    dk = tn(dqk, q) + nn(dg, k) + tn(dg, k) + dkg + dkd
    kept = jnp.sum(dkd * k, axis=1, keepdims=True)
    gcol = jnp.sum(logs, axis=1, keepdims=True) + jnp.sum(dqd * q + dkg * k, axis=1, keepdims=True) - kept
    last = jnp.sum(kept, axis=0, keepdims=True) + jnp.exp(ge) * jnp.sum(
        jnp.sum(start * end, axis=1, keepdims=True), axis=0, keepdims=True
    )
    rows = lax.broadcasted_iota(jnp.int32, gcol.shape, 0)
    gcol = gcol + jnp.where(rows == gcol.shape[0] - 1, last, 0.0)
    grow = jnp.sum(logs, axis=0, keepdims=True)
    dqr = (rq * scale) * (dq - qr * (rq * rq * jnp.sum(qr * dq, axis=1, keepdims=True)))
    dkr = rk * (dk - kr * (rk * rk * jnp.sum(kr * dk, axis=1, keepdims=True)))
    return dqr, dkr, db, gcol, grow


def pick(ref, head):
    table = ref[...]
    lane = lax.broadcasted_iota(jnp.int32, table.shape, 1)
    return jnp.sum(jnp.where(lane == head, table, 0.0), axis=1, keepdims=True)


def put(ref, head, column):
    lane = lax.broadcasted_iota(jnp.int32, ref.shape, 1)
    ref[...] = jnp.where(lane == head, column, ref[...])


def gains(g_ref, row_ref, head):
    gr = row_ref[...]
    return pick(g_ref, head), gr, gr[:, gr.shape[1] - 1 :]


def lanes(ref, i, group):
    width = ref.shape[1] // group
    return ref.at[:, i * width : (i + 1) * width]


def first_kernel(group, q, k, v, do, b, g, row, inv_o, uw_o, dw_o, t_o, off_o, own_o):
    results = []
    for i in range(group):
        head = pl.program_id(0) * group + i
        gc, gr, ge = gains(g, row.at[i], head)
        results.append(
            [lanes(a, i, group)[...].astype(f32) for a in (q, k, v, do)]
            + [pick(b, head), gc, gr, ge]
        )
    results = first_phase_group(results)
    for i in range(group):
        inverse, uw, dw0, transition, offset, own = results[i]
        inv_o[i] = inverse.astype(inv_o.dtype)
        uw_o[i] = uw
        dw_o[i] = dw0
        t_o[i] = transition.astype(bf16)
        off_o[i] = offset.astype(bf16)
        own_o[i] = own.astype(bf16)


def value_kernel(group, k, inv, dw, end, b, g, row, dr_o, dv_o):
    for i in range(group):
        head = pl.program_id(0) * group + i
        gc, _, ge = gains(g, row.at[i], head)
        bc = pick(b, head)
        dr = value_phase(lanes(k, i, group)[...].astype(f32), inv[i], dw[i], end[i], gc, ge)
        dr_o[i] = dr
        lanes(dv_o, i, group)[...] = (bc * dr).astype(bf16)


def last_kernel(group, q, k, v, do, uw, dr, start, end, b, g, row, dq_o, dk_o, db_o, gc_o, gr_o):
    @pl.when(pl.program_id(0) == 0)
    def _():
        db_o[...] = jnp.zeros_like(db_o)
        gc_o[...] = jnp.zeros_like(gc_o)

    for i in range(group):
        head = pl.program_id(0) * group + i
        gc, gr, ge = gains(g, row.at[i], head)
        raw = [lanes(a, i, group)[...].astype(f32) for a in (q, k, v, do)]
        dqr, dkr, db, gcol, grow = last_phase(
            *raw, uw[i], dr[i], start[i].astype(f32), end[i].astype(f32), pick(b, head), gc, gr, ge
        )
        lanes(dq_o, i, group)[...] = dqr.astype(bf16)
        lanes(dk_o, i, group)[...] = dkr.astype(bf16)
        put(db_o, head, db)
        put(gc_o, head, gcol)
        gr_o[i] = grow


def scan_kernel(count, t, off, own, start_o, end_o):
    shape = off.shape[1:]

    def split(a, b, ca):
        hi = b.astype(bf16)
        return mm(a, hi, ca, 0) + mm(a, b - hi.astype(f32), ca, 0)

    def step(i, carry):
        state, grad = carry
        j = count - 1 - i
        start_o[i] = state.astype(bf16)
        end_o[j] = grad.astype(bf16)
        state = split(t[i], state, 1) + off[i].astype(f32)
        grad = split(t[j], grad, 0) + own[j].astype(f32)
        return state, grad

    zero = jnp.zeros(shape, f32)
    lax.fori_loop(0, count, step, (zero, zero))


def exchange(value, axis, bit):
    count = lax.axis_size(axis)
    return lax.ppermute(value, axis, [(i, i ^ bit) for i in range(count)])


def bit_of(axis, bit):
    return (lax.axis_index(axis) >> bit) & 1


class Halving:
    def __init__(self, hidden, grads, bits, sequence):
        self.grads, self.sequence = grads, sequence
        self.length, self.rows, self.count = hidden.shape[0], hidden.shape[1], 1 << bits
        self.left = sorted(range(bits), reverse=True)
        self.axis = 1 + self.left.index(sequence[0])
        self.mine = bit_of("sp", sequence[0])
        self.split = hidden.reshape((self.length,) + (2,) * bits + (self.rows // self.count,))
        self.send = self.product(1 - self.mine).astype(bf16)

    def product(self, side):
        piece = lax.dynamic_index_in_dim(self.split, side, self.axis, False)
        piece = piece.reshape(self.length, self.rows // 2)
        return lax.dot_general(
            piece, self.grads, (((0,), (0,)), ((), ())), preferred_element_type=f32
        )

    def finish(self, send):
        left = list(self.left)
        got = exchange(send, "sp", 1 << self.sequence[0])
        total = self.product(self.mine) + got.astype(f32)
        left.remove(self.sequence[0])
        for bit in self.sequence[1:]:
            place = left.index(bit)
            mine = bit_of("sp", bit)
            shaped = total.reshape(1 << place, 2, -1, total.shape[-1])
            send = lax.dynamic_index_in_dim(shaped, 1 - mine, 1, False)
            keep = lax.dynamic_index_in_dim(shaped, mine, 1, False)
            got = exchange(send.astype(bf16), "sp", 1 << bit)
            total = keep + got.astype(f32)
            left.remove(bit)
        return total.reshape(self.rows // self.count, -1)


def plan_weight(hidden, grads, count):
    bits = count.bit_length() - 1
    low = bits // 2
    order_a = list(range(bits))
    order_b = order_a[:low][::-1] + order_a[low:]
    order_c = order_a[low:] + order_a[:low]
    width = grads.shape[1]
    cut = max(width * 3 // 8 // 128 * 128, 1)
    groups = [(0, cut, order_a), (cut, 2 * cut, order_b), (2 * cut, width, order_c)]
    return [Halving(hidden, grads[:, lo:hi], bits, seq) for lo, hi, seq in groups]


def reduce_hidden(grads, weight):
    cores = lax.axis_size("tp")
    assert cores == 2
    half = grads.shape[0] // cores
    me = lax.axis_index("tp")

    def product(side):
        rows = lax.dynamic_slice_in_dim(grads, side * half, half, 0)
        return lax.dot_general(
            rows, weight, (((1,), (1,)), ((), ())), preferred_element_type=f32
        ).astype(bf16)

    send = product(1 - me)
    got = exchange(send, "tp", 1)
    return (product(me).astype(f32) + got.astype(f32)).astype(bf16)


def compute(queries, keys, hidden, value_weight, beta_pre, decay_pre, decay_rate, out_grad):
    heads = decay_rate.shape[0]
    length, dk = queries.shape[0], queries.shape[1] // heads
    dv = value_weight.shape[1] // heads
    count = lax.axis_size("sp")
    parts = count // heads
    group = 4 if heads % 4 == 0 else 1
    cols = dv // parts

    values = jnp.dot(hidden, value_weight, preferred_element_type=f32).astype(bf16)
    beta = jax.nn.sigmoid(beta_pre)
    log_decay = -decay_rate[None, :] * jax.nn.softplus(decay_pre)
    inclusive = jnp.tril(jnp.ones((length, length), f32))
    sums = jnp.dot(inclusive, log_decay, precision=lax.Precision.HIGHEST)
    sums_row = sums.T.reshape(heads, 1, length)

    wide = lambda n: pl.BlockSpec((length, group * n), lambda h: (0, h))
    per_head = lambda r, c: pl.BlockSpec((group, r, c), lambda h: (h, 0, 0))
    table = pl.BlockSpec((length, heads), lambda h: (0, 0))
    shape = jax.ShapeDtypeStruct
    params = pltpu.CompilerParams(dimension_semantics=("arbitrary",))

    inverse, uw, dw0, transition, offset, own = pl.pallas_call(
        functools.partial(first_kernel, group),
        grid=(heads // group,),
        in_specs=[wide(dk), wide(dk), wide(dv), wide(dv), table, table, per_head(1, length)],
        out_specs=[
            per_head(length, length), per_head(length, dv + dk), per_head(length, dv),
            per_head(dk, dk), per_head(dk, dv), per_head(dk, dv),
        ],
        out_shape=[
            shape((heads, length, length), bf16), shape((heads, length, dv + dk), f32),
            shape((heads, length, dv), f32), shape((heads, dk, dk), bf16),
            shape((heads, dk, dv), bf16), shape((heads, dk, dv), bf16),
        ],
        compiler_params=params,
        name="first",
    )(queries, keys, values, out_grad, beta, sums, sums_row)

    def by_owner(a):
        a = a.reshape(heads, dk, parts, cols)
        return jnp.moveaxis(a, 2, 1).reshape(count, dk, cols)

    packed = jnp.concatenate(
        [jnp.repeat(transition, parts, axis=0), by_owner(offset), by_owner(own)], axis=2
    )
    got = lax.all_to_all(packed, "sp", 0, 0, tiled=True)
    starts, ends = pl.pallas_call(
        functools.partial(scan_kernel, count),
        out_shape=[shape((count, dk, cols), bf16), shape((count, dk, cols), bf16)],
        name="scan",
    )(got[:, :, :dk], got[:, :, dk : dk + cols], got[:, :, dk + cols :])
    back = lax.all_to_all(jnp.concatenate([starts, ends], axis=2), "sp", 0, 0, tiled=True)
    back = jnp.moveaxis(back.reshape(heads, parts, dk, 2, cols), 1, 3).reshape(heads, dk, 2, dv)
    start, end = back[:, :, 0], back[:, :, 1]

    dr, grad_values = pl.pallas_call(
        functools.partial(value_kernel, group),
        grid=(heads // group,),
        in_specs=[
            wide(dk), per_head(length, length), per_head(length, dv), per_head(dk, dv),
            table, table, per_head(1, length),
        ],
        out_specs=[per_head(length, dv), wide(dv)],
        out_shape=[shape((heads, length, dv), f32), shape((length, heads * dv), bf16)],
        compiler_params=params,
        name="value",
    )(keys, inverse, dw0, end, beta, sums, sums_row)

    plans = plan_weight(hidden, grad_values, count)
    sends, dr, start = lax.optimization_barrier(([plan.send for plan in plans], dr, start))
    d_weight = jnp.concatenate([plan.finish(x) for plan, x in zip(plans, sends)], axis=1)
    d_hidden = reduce_hidden(grad_values, value_weight)

    d_queries, d_keys, db, gcol, grow = pl.pallas_call(
        functools.partial(last_kernel, group),
        grid=(heads // group,),
        in_specs=[
            wide(dk), wide(dk), wide(dv), wide(dv), per_head(length, dv + dk),
            per_head(length, dv), per_head(dk, dv), per_head(dk, dv),
            table, table, per_head(1, length),
        ],
        out_specs=[wide(dk), wide(dk), table, table, per_head(1, length)],
        out_shape=[
            shape(queries.shape, bf16), shape(keys.shape, bf16), shape((length, heads), f32),
            shape((length, heads), f32), shape((heads, 1, length), f32),
        ],
        compiler_params=params,
        cost_estimate=pl.CostEstimate(
            flops=heads * 13 * 2 * length * length * dk, bytes_accessed=12 << 20, transcendentals=0
        ),
        name="last",
    )(queries, keys, values, out_grad, uw, dr, start, end, beta, sums, sums_row)
    grad_sums = gcol - grow.reshape(heads, length).T
    grad_log = jnp.dot(inclusive.T, grad_sums, precision=lax.Precision.HIGHEST)
    d_decay = grad_log * (-decay_rate[None, :] * jax.nn.sigmoid(decay_pre))
    d_beta = db * beta * (1.0 - beta)
    return (d_queries, d_keys, d_beta, d_decay, d_hidden, d_weight)


def solution(mesh):
    return jax.shard_map(
        compute,
        mesh=mesh,
        in_specs=(
            P("sp", "tp"), P("sp", "tp"), P("sp", None), P(None, "tp"),
            P("sp", "tp"), P("sp", "tp"), P("tp"), P("sp", "tp"),
        ),
        out_specs=(
            P("sp", "tp"), P("sp", "tp"), P("sp", "tp"), P("sp", "tp"),
            P(("sp", "tp"), None), P("sp", "tp"),
        ),
        check_vma=False,
    )
```
